32 devices in a mesh: sp: 8 (over z, y), dp: 4 (over x, core).
Axes of the slice: x: 2, y: 2, z: 4, core: 2. Of those that a mesh axis runs over, the one named last changes fastest.
Arguments:
- query_weight: bfloat16 [4, 3072, 1024], P('dp', 'sp'), may hold values from -6 to 6
- forget_preactivation: bfloat16 [4, 3072, 1024], P('dp', 'sp'), may hold values from -7 to 7
- written_input: bfloat16 [4, 3072, 1024], P('dp', 'sp'), may hold values from -6 to 6
- output_gate_logit: bfloat16 [4, 3072, 1024], P('dp', 'sp'), may hold values from -6 to 6
- forget_floor: float32 [1024], replicated, may hold values from 0.9 to 1
- extra_log_decay: float32 [4, 3072, 16], P('dp'), may hold values from -0.7 to 0
- residual: bfloat16 [4, 3072, 2048], P('dp', 'sp'), may hold values from -6 to 6
- output_weight: bfloat16 [1024, 2048], P('dp'), may hold values from -0.1875 to 0.1875
- norm_scale_vector: float32 [2048], replicated, may hold values from 0.1 to 1.9
- expert_gate_weight: bfloat16 [8, 2048, 1024], P('sp'), may hold values from -0.125 to 0.125
- expert_up_weight: bfloat16 [8, 2048, 1024], P('sp'), may hold values from -0.125 to 0.125
- expert_down_weight: bfloat16 [8, 1024, 2048], P('sp'), may hold values from -0.1875 to 0.1875
- routes: int32 [4, 3072, 2], P('dp', 'sp'), may hold values from 0 to 7, as said below
- routing_weight: float32 [4, 3072, 2], P('dp', 'sp'), may hold values from 0.2 to 1
Outputs:
- layer_out: bfloat16 [4, 3072, 2048], P('dp', 'sp')
The draws below stay inside these ranges and needn't reach their ends.
Inputs may be any that keep to these rules, and one draw needn't show every extreme that they name: `routes`: the two experts of a position differ and lie in one group of four, 4 g to 4 g + 3. In the positions of one device no expert is named more than 192 times. In every draw one expert is named exactly 192 times by the positions of every device, and on some devices each of the four experts of one group is named exactly 192 times.
All inputs are finite; a program needn't handle non-finite values.
Results may differ from the reference program's by a relative error of at most 0.0059.
Values may be sent and summed in bfloat16 or wider, within the bound.
A program may use at most 128 MiB of HBM per device.

```python
import math
import jax
import jax.numpy as jnp
from jax import lax

D = 2048
RECURRENT_HEADS = 16
HEAD_CHANNELS = 64
W = 1024
DE = 1024
BLOCK = 64
TOK_DEV = 384
SEQS = 4
LEN = 3072
EXPERTS = 8
GROUPS = 2
CAP = 192
N_SP = 8


def draw_forget_preactivation(key, part):
    subkeys = jax.random.split(jax.random.fold_in(key, 3), 2)
    jitter = jnp.clip(jax.random.normal(subkeys[0], (SEQS, LEN, RECURRENT_HEADS, HEAD_CHANNELS), jnp.float32), -5.0, 5.0)
    shards = LEN // TOK_DEV
    shifts = jax.random.uniform(subkeys[1], (SEQS, shards, 1, RECURRENT_HEADS, 1), jnp.float32, -1.2, 1.2)
    values = jitter.reshape(SEQS, shards, TOK_DEV, RECURRENT_HEADS, HEAD_CHANNELS) + shifts
    return values.reshape(SEQS, LEN, W).astype(jnp.bfloat16)


def draw_forget_floor(key, part):
    subkeys = jax.random.split(jax.random.fold_in(key, 5), 4)
    share = 0.5
    slow = jax.random.bernoulli(subkeys[0], share, (RECURRENT_HEADS, 1))
    slow_rate = jnp.exp(jax.random.uniform(subkeys[1], (RECURRENT_HEADS, 1), jnp.float32, math.log(0.15), math.log(1.2))) / LEN
    fast_rate = jnp.exp(jax.random.uniform(subkeys[2], (RECURRENT_HEADS, 1), jnp.float32, math.log(0.04), math.log(0.1)))
    channel = jnp.exp(jax.random.uniform(subkeys[3], (RECURRENT_HEADS, HEAD_CHANNELS), jnp.float32, math.log(0.5), 0.0))
    rates = jnp.where(slow, slow_rate, fast_rate) * channel
    return (1.0 - rates).reshape(W).astype(jnp.float32)


def draw_extra_log_decay(key, part):
    subkeys = jax.random.split(jax.random.fold_in(key, 9), 2)
    places = jax.random.randint(subkeys[0], (SEQS, 3), 0, LEN)
    depth = jnp.log(jax.random.uniform(subkeys[1], (SEQS, 3, RECURRENT_HEADS), jnp.float32, 0.5, 0.8))
    marks = (jnp.arange(LEN)[None, :, None] == places[:, None, :]).astype(jnp.float32)
    return jnp.einsum('slb,sbh->slh', marks, depth).astype(jnp.float32)


def draw_routes(key, part):
    blocks_all = SEQS * LEN // TOK_DEV
    others = GROUPS - 1
    subkeys = jax.random.split(jax.random.fold_in(key, 13), 9)
    busiest = jax.random.randint(subkeys[0], (), 0, EXPERTS)
    hot_group = busiest // 4
    hot_local = busiest % 4
    spread = jax.random.randint(subkeys[1], (blocks_all, others), 0, CAP // 4 + 1)
    counts = CAP + spread - jnp.roll(spread, -1, axis=1)
    group_ends = jnp.cumsum(counts, axis=1)
    rotate = jax.random.randint(subkeys[2], (blocks_all, 1), 0, others)
    offset = jax.random.randint(subkeys[3], (blocks_all, GROUPS), 0, 4)
    places = jnp.broadcast_to(jnp.arange(TOK_DEV)[None, :], (blocks_all, TOK_DEV))
    remain = places - CAP
    slot_group = jnp.sum((remain[:, :, None] >= group_ends[:, None, :]).astype(jnp.int32), axis=2)
    slot_group = jnp.minimum(slot_group, others - 1)
    group_starts = jnp.take_along_axis(group_ends - counts, slot_group, axis=1)
    inside = remain - group_starts
    other_group = (hot_group + 1 + (slot_group + rotate) % others) % GROUPS
    shift_by = jnp.take_along_axis(offset, other_group, axis=1)
    primary_other = other_group * 4 + (inside + shift_by) % 4
    secondary_other = other_group * 4 + (inside + shift_by + 1) % 4
    secondary_hot = hot_group * 4 + (hot_local + 1 + places % 3) % 4
    is_hot = places < CAP
    drawn_primary = jnp.where(is_hot, busiest, primary_other)
    drawn_secondary = jnp.where(is_hot, secondary_hot, secondary_other)
    matching = jax.random.randint(subkeys[6], (blocks_all,), 0, 3)
    table = jnp.array([[0, 1, 2, 3], [0, 2, 1, 3], [0, 3, 1, 2]], jnp.int32)
    pairing = table[matching]
    parity = places % 2
    first_local = jnp.take_along_axis(pairing, 2 * parity, axis=1)
    second_local = jnp.take_along_axis(pairing, 2 * parity + 1, axis=1)
    leftover = jnp.maximum(places - 2 * CAP, 0)
    leftover_group = (hot_group + 1 + (leftover + rotate) % others) % GROUPS
    leftover_shift = jnp.take_along_axis(offset, leftover_group, axis=1)
    within = leftover // others
    in_full = places < 2 * CAP
    full_primary = jnp.where(in_full, hot_group * 4 + first_local, leftover_group * 4 + (within + leftover_shift) % 4)
    full_secondary = jnp.where(in_full, hot_group * 4 + second_local, leftover_group * 4 + (within + leftover_shift + 1) % 4)
    chosen = jax.random.randint(subkeys[7], (blocks_all, 1), 0, 2)
    forced = jax.random.randint(subkeys[8], (), 0, blocks_all)
    block_index = jnp.arange(blocks_all, dtype=jnp.int32)[:, None]
    full_block = jnp.where(block_index == forced, 1, jnp.where(block_index == (forced + 1) % blocks_all, 0, chosen))
    primary = jnp.where(full_block == 1, full_primary, drawn_primary)
    secondary = jnp.where(full_block == 1, full_secondary, drawn_secondary)
    scores = jax.random.randint(subkeys[4], (blocks_all, TOK_DEV), 0, TOK_DEV) * TOK_DEV + places
    shuffle = jnp.argsort(scores, axis=1)
    primary = jnp.take_along_axis(primary, shuffle, axis=1)
    secondary = jnp.take_along_axis(secondary, shuffle, axis=1)
    flipped = jax.random.randint(subkeys[5], (blocks_all, TOK_DEV, 1), 0, 2)
    straight = jnp.stack([primary, secondary], axis=2)
    crossed = jnp.stack([secondary, primary], axis=2)
    paired = jnp.where(flipped == 1, crossed, straight)
    return paired.reshape(SEQS, LEN, 2).astype(jnp.int32)


def levels(rng, dims, cuts, low, largest):
    level = 1.0
    for dim, blocks in cuts:
        heights = jax.random.uniform(jax.random.fold_in(jax.random.fold_in(rng, 6), dim), (blocks,), jnp.float32, low / len(cuts), largest / len(cuts))
        level = level * jnp.repeat(jnp.exp(heights), dims[dim] // blocks).reshape((-1,) + (1,) * (len(dims) - 1 - dim))
    return level


def scatter_about(key, shape, deviation, limit, pieces=(), held_as=jnp.bfloat16):
    gain = levels(key, shape, pieces, -0.22, 0.18) if pieces else 1.0
    values = jax.random.normal(key, shape, jnp.float32) * deviation * gain
    return jnp.minimum(jnp.maximum(values, -limit), limit).astype(held_as)


def setup_inputs(seed: int = 0) -> dict:
    seeds = jax.random.split(jax.random.key(seed), 15)
    return {
        "query_weight": scatter_about(seeds[0], (SEQS, LEN, W), 1.0, 6.0, ((0, 4), (1, 8))),
        "forget_preactivation": draw_forget_preactivation(jax.random.fold_in(seeds[14], 71), 0),
        "written_input": scatter_about(seeds[2], (SEQS, LEN, W), 1.0, 6.0, ((0, 4), (1, 8))),
        "output_gate_logit": scatter_about(seeds[3], (SEQS, LEN, W), 1.0, 6.0, ((0, 4), (1, 8))),
        "forget_floor": draw_forget_floor(jax.random.fold_in(seeds[14], 71), 0),
        "extra_log_decay": draw_extra_log_decay(jax.random.fold_in(seeds[14], 71), 0),
        "residual": scatter_about(seeds[6], (SEQS, LEN, D), 1.0, 6.0, ((0, 4), (1, 8))),
        "output_weight": scatter_about(seeds[7], (W, D), W ** -0.5, 0.1875, ((0, 4),)),
        "norm_scale_vector": jnp.clip(1.0 + 0.18 * jax.random.normal(seeds[8], (D,), jnp.float32), 0.1, 1.9),
        "expert_gate_weight": scatter_about(seeds[9], (EXPERTS, D, DE), D ** -0.5, 0.125, ((0, 8),)),
        "expert_up_weight": scatter_about(seeds[10], (EXPERTS, D, DE), D ** -0.5, 0.125, ((0, 8),)),
        "expert_down_weight": scatter_about(seeds[11], (EXPERTS, DE, D), DE ** -0.5, 0.1875, ((0, 8),)),
        "routes": draw_routes(jax.random.fold_in(seeds[14], 71), 0),
        "routing_weight": jnp.clip(0.2 + 0.8 * jax.random.uniform(seeds[13], (SEQS, LEN, 2), jnp.float32) ** levels(seeds[13], (SEQS, LEN, 2), ((0, 4), (1, 8)), -0.2, 0.2), 0.2, 1.0),
    }


HIGHEST = lax.Precision.HIGHEST

def head_norm(values):
    return values * lax.rsqrt(lax.optimization_barrier(jnp.mean(values * values, axis=-1, keepdims=True)) + 1e-06)

def linear_recurrent(query_unprojected, forget_unbounded, value_unprojected, floor_level, decay_spikes, prefixed_state):
    seq_count, length, head_count, channels = query_unprojected.shape
    block_count = length // BLOCK
    queries = jax.nn.silu(query_unprojected)
    forget_logarithm = jnp.logaddexp(jnp.log(floor_level), jnp.log1p(-floor_level) + jax.nn.log_sigmoid(forget_unbounded)) + decay_spikes[..., None]
    keys_in = (1.0 - floor_level) * jax.nn.sigmoid(-forget_unbounded)

    def to_blocks(tensor):
        return tensor.reshape(seq_count, block_count, BLOCK, head_count, channels).transpose(1, 0, 3, 2, 4)
    q_blocks = to_blocks(queries)
    k_blocks = to_blocks(keys_in)
    v_blocks = to_blocks(value_unprojected)
    cumulative = jnp.cumsum(to_blocks(forget_logarithm), axis=3)
    causal = jnp.tril(jnp.ones((BLOCK, BLOCK), bool))[:, :, None]

    def advance(states, inputs):
        block_q, block_k, block_v, block_b = inputs
        spread_log = block_b[:, :, :, None, :] - block_b[:, :, None, :, :]
        decays = jnp.where(causal, jnp.exp(jnp.where(causal, spread_log, 0.0)), 0.0)
        scores = jnp.einsum('bhtk,bhsk,bhtsk->bhts', block_q, block_k, decays, precision=HIGHEST)
        outputs = jnp.einsum('bhts,bhsv->bhtv', scores, block_v, precision=HIGHEST)
        outputs = outputs + jnp.einsum('bhtk,bhkv->bhtv', block_q * jnp.exp(block_b), states, precision=HIGHEST)
        closing = block_b[:, :, -1:, :]
        states = jnp.exp(closing[:, :, 0, :, None]) * states + jnp.einsum('bhsk,bhsv->bhkv', block_k * jnp.exp(closing - block_b), block_v, precision=HIGHEST)
        return (states, outputs)
    initial = jnp.zeros((seq_count, head_count, channels, channels), jnp.float32)
    states, outputs = lax.scan(advance, initial, (q_blocks, k_blocks, v_blocks, cumulative))
    final_output = outputs.transpose(1, 0, 3, 2, 4).reshape(seq_count, length, head_count, channels)
    if prefixed_state:
        totals = cumulative[:, :, :, -1, :]
        before = jnp.cumsum(totals, axis=0) - totals
        running = (cumulative + before[:, :, :, None, :]).transpose(1, 0, 3, 2, 4)
        running = running.reshape(seq_count, length, head_count, channels)
        return (final_output, states, running, queries)
    return (final_output, states, None, queries)

def reference(query_weight, forget_preactivation, written_input, output_gate_logit, forget_floor, extra_log_decay, residual, output_weight, norm_scale_vector, expert_gate_weight, expert_up_weight, expert_down_weight, routes, routing_weight):

    def divide_into_heads(tensor):
        return tensor.astype(jnp.float32).reshape(SEQS, LEN, RECURRENT_HEADS, HEAD_CHANNELS)
    final_output, unused_item, unused_item, unused_item = linear_recurrent(divide_into_heads(query_weight), divide_into_heads(forget_preactivation), divide_into_heads(written_input), forget_floor.reshape(RECURRENT_HEADS, HEAD_CHANNELS), extra_log_decay, False)
    mixer_out = (head_norm(final_output) * jax.nn.silu(divide_into_heads(output_gate_logit))).astype(jnp.bfloat16)
    total_rows = SEQS * LEN
    mixer_out = mixer_out.reshape(total_rows, W)
    updated = (residual.reshape(total_rows, D).astype(jnp.float32) + jnp.dot(mixer_out, output_weight, preferred_element_type=jnp.float32)).astype(jnp.bfloat16)
    widened = lax.optimization_barrier(updated).astype(jnp.float32)
    normed = (widened * lax.rsqrt(lax.optimization_barrier(jnp.mean(widened * widened, axis=-1, keepdims=True)) + 1e-06) * norm_scale_vector.astype(jnp.float32)).astype(jnp.bfloat16)
    padded = jnp.concatenate([normed, jnp.zeros((1, D), jnp.bfloat16)], axis=0)
    picks = jnp.concatenate([routes.reshape(-1), jnp.full((1,), -1, jnp.int32)])
    weights = jnp.concatenate([routing_weight.reshape(-1), jnp.zeros((1,), jnp.float32)])
    bound_rows = SEQS * N_SP * CAP

    def serve(summed, expert):
        found = jnp.nonzero(picks == expert, size=bound_rows, fill_value=2 * total_rows)[0].astype(jnp.int32)
        tokens_hit = found // 2
        picked = padded[tokens_hit]
        gated = jnp.dot(picked, expert_gate_weight[expert], preferred_element_type=jnp.float32)
        upward = jnp.dot(picked, expert_up_weight[expert], preferred_element_type=jnp.float32)
        hidden = (jax.nn.silu(gated) * upward).astype(jnp.bfloat16)
        produced = jnp.dot(hidden, expert_down_weight[expert], preferred_element_type=jnp.float32).astype(jnp.bfloat16)
        produced = lax.optimization_barrier(produced).astype(jnp.float32)
        summed = summed.at[tokens_hit].add(weights[found][:, None] * produced)
        return (summed, None)
    summed, unused_item = lax.scan(serve, jnp.zeros((total_rows + 1, D), jnp.float32), jnp.arange(EXPERTS, dtype=jnp.int32))
    layer_out = (widened + summed[:total_rows]).astype(jnp.bfloat16)
    return layer_out.reshape(SEQS, LEN, D)
```

```python
import functools

import jax
import jax.numpy as jnp
from jax import lax
from jax.experimental import pallas as pl
from jax.experimental.pallas import tpu as pltpu
from jax.sharding import PartitionSpec as P

HEAD_CHANNELS = 64
BLOCK = 64
PAIR = 2 * HEAD_CHANNELS
STATE_ROWS = 80
GROUP = 4
HIGHEST = lax.Precision.HIGHEST


def dot_f32(a, b, dims=((1,), (0,))):
    return lax.dot_general(
        a, b, (dims, ((), ())), precision=HIGHEST, preferred_element_type=jnp.float32
    )


def iota(shape, axis):
    return lax.broadcasted_iota(jnp.int32, shape, axis)


def dot_bf16(a, b, dims=((1,), (0,))):
    return lax.dot_general(
        a.astype(jnp.bfloat16),
        b.astype(jnp.bfloat16),
        (dims, ((), ())),
        preferred_element_type=jnp.float32,
    )


def three_parts(value):
    high = value.astype(jnp.bfloat16)
    rest = value - high.astype(jnp.float32)
    middle = rest.astype(jnp.bfloat16)
    low = (rest - middle.astype(jnp.float32)).astype(jnp.bfloat16)
    return high, middle, low


def mixer_kernel(
    devices,
    q_ref,
    f_ref,
    v_ref,
    gate_ref,
    floor_ref,
    extra_ref,
    out_ref,
    local_ref,
    decayed_ref,
    send_ref,
    recv_ref,
    earlier_ref,
    earlier_log_ref,
    upto_ref,
    upto_log_ref,
    send_sem,
    recv_sem,
):
    rows = q_ref.shape[1]
    pairs = local_ref.shape[0]
    rounds = send_ref.shape[0]
    heads = extra_ref.shape[1] // 3
    step = pl.program_id(0)
    place = lax.axis_index("sp")
    first = iota((1, PAIR), 1) < HEAD_CHANNELS

    def copy(number, pair):
        return pltpu.make_async_remote_copy(
            src_ref=send_ref.at[number, pair],
            dst_ref=recv_ref.at[number, pair],
            send_sem=send_sem.at[number, pair],
            recv_sem=recv_sem.at[number, pair],
            device_id={"sp": lax.rem(place + 2**number, devices)},
            device_id_type=pl.DeviceIdType.MESH,
        )

    def pack(number, pair, state, total):
        high, middle, low = three_parts(total)
        row = iota((STATE_ROWS - HEAD_CHANNELS, PAIR), 0)
        logs = jnp.where(
            row == 0,
            high.astype(jnp.float32),
            jnp.where(
                row == 1,
                middle.astype(jnp.float32),
                jnp.where(row == 2, low.astype(jnp.float32), 0.0),
            ),
        )
        send_ref[number, pair] = jnp.concatenate([state, logs], axis=0).astype(jnp.bfloat16)

    @pl.when(step == 0)
    def _():
        barrier = pltpu.get_barrier_semaphore()
        for number in range(rounds):
            for other in (place + 2**number, place + devices - 2**number):
                pl.semaphore_signal(
                    barrier,
                    inc=1,
                    device_id={"sp": lax.rem(other, devices)},
                    device_id_type=pl.DeviceIdType.MESH,
                )
        pl.semaphore_wait(barrier, 2 * rounds)

    @pl.when(step < pairs)
    def _():
        pair = step
        blocks = rows // BLOCK
        spread = (
            iota((3 * heads, PAIR), 0) % heads
            == 2 * pair + iota((3 * heads, PAIR), 1) // HEAD_CHANNELS
        ).astype(jnp.float32)
        extra = dot_bf16(extra_ref[...], spread)
        same_head = (
            iota((PAIR, PAIR), 0) // HEAD_CHANNELS == iota((PAIR, PAIR), 1) // HEAD_CHANNELS
        )
        lower = (iota((BLOCK, 3 * BLOCK), 0) >= iota((BLOCK, 3 * BLOCK), 1) % BLOCK).astype(
            jnp.float32
        )
        causal = iota((2 * BLOCK, BLOCK), 0) % BLOCK >= iota((2 * BLOCK, BLOCK), 1)
        open_share = 1.0 - floor_ref[...]
        keys = []
        logs = []
        for block in range(blocks):
            at = slice(block * BLOCK, (block + 1) * BLOCK)
            k = open_share / (1.0 + jnp.exp(f_ref[0, at, :].astype(jnp.float32)))
            keys.append(k)
            logs.append(
                jnp.concatenate(three_parts(jnp.log1p(-k) + extra[at]), axis=0)
            )
        sums = dot_bf16(lower, jnp.concatenate(logs, axis=1))
        state = jnp.zeros((PAIR, PAIR), jnp.float32)
        before = jnp.zeros((1, PAIR), jnp.float32)
        for block in range(blocks):
            at = slice(block * BLOCK, (block + 1) * BLOCK)
            q = q_ref[0, at, :].astype(jnp.float32)
            v = v_ref[0, at, :]
            k = keys[block]
            q = q / (1.0 + jnp.exp(-q))
            cumulative = sums[:, block * PAIR : (block + 1) * PAIR]
            closing = cumulative[BLOCK - 1 :, :]
            q_decayed = q * jnp.exp(cumulative)
            k_grown = k * jnp.exp(-cumulative)
            k_closing = k * jnp.exp(closing - cumulative)
            stacked = jnp.concatenate(
                [jnp.where(first, q_decayed, 0.0), jnp.where(first, 0.0, q_decayed)], axis=0
            )
            scores = jnp.where(causal, dot_bf16(stacked, k_grown, ((1,), (1,))), 0.0)
            inner = dot_bf16(scores, v)
            inner = jnp.where(first, inner[:BLOCK], inner[BLOCK:])
            local_ref[pair, at, :] = inner + dot_bf16(q_decayed, state, ((1,), (1,)))
            decayed_ref[pair, at, :] = (q_decayed * jnp.exp(before)).astype(jnp.bfloat16)
            state = state * jnp.exp(closing) + jnp.where(
                same_head, dot_bf16(v, k_closing, ((0,), (0,))), 0.0
            )
            before = before + closing
        folded = jnp.where(first, state[:HEAD_CHANNELS], state[HEAD_CHANNELS:])
        upto_ref[pair] = folded
        upto_log_ref[pair] = jnp.broadcast_to(before, (8, PAIR))
        earlier_ref[pair] = jnp.zeros((HEAD_CHANNELS, PAIR), jnp.float32)
        earlier_log_ref[pair] = jnp.zeros((8, PAIR), jnp.float32)

        @pl.when(place + 1 < devices)
        def _():
            pack(0, pair, folded, before)
            copy(0, pair).start()

    def merge(number):
        distance = 2**number
        pair = step - 1 - number

        @pl.when((pair >= 0) & (pair < pairs))
        def _():
            @pl.when(place >= distance)
            def _():
                copy(number, pair).wait_recv()
                item = recv_ref[number, pair].astype(jnp.float32)
                state = item[:HEAD_CHANNELS]
                total = jnp.sum(item[HEAD_CHANNELS:], axis=0, keepdims=True)
                log = earlier_log_ref[pair][:1]
                earlier_ref[pair] = state * jnp.exp(log) + earlier_ref[pair]
                earlier_log_ref[pair] = jnp.broadcast_to(log + total, (8, PAIR))
                if number + 1 < rounds:
                    log = upto_log_ref[pair][:1]
                    upto_ref[pair] = state * jnp.exp(log) + upto_ref[pair]
                    upto_log_ref[pair] = jnp.broadcast_to(log + total, (8, PAIR))

            if number + 1 < rounds:

                @pl.when(place + 2 * distance < devices)
                def _():
                    pack(number + 1, pair, upto_ref[pair], upto_log_ref[pair][:1])
                    copy(number + 1, pair).start()

    for number in range(rounds):
        merge(number)

    pair = step - rounds

    @pl.when(pair >= 0)
    def _():
        state = earlier_ref[pair]
        state = jnp.concatenate(
            [jnp.where(first, state, 0.0), jnp.where(first, 0.0, state)], axis=0
        )
        value = local_ref[pair] + dot_bf16(decayed_ref[pair], state, ((1,), (1,)))
        same_head = (
            iota((2 * PAIR, PAIR), 0) // HEAD_CHANNELS % 2 == iota((2 * PAIR, PAIR), 1) // HEAD_CHANNELS
        ).astype(jnp.float32)
        square = value * value
        high = square.astype(jnp.bfloat16)
        low = (square - high.astype(jnp.float32)).astype(jnp.bfloat16)
        mean = dot_bf16(jnp.concatenate([high, low], axis=1), same_head) * (1.0 / HEAD_CHANNELS)
        gate = gate_ref[0].astype(jnp.float32)
        gate = gate / (1.0 + jnp.exp(-gate))
        out_ref[...] = (value * lax.rsqrt(mean + 1e-06) * gate).astype(jnp.bfloat16)

    @pl.when(step == pairs + rounds - 1)
    def _():
        for number in range(rounds):

            @pl.when(place + 2**number < devices)
            def _():
                for pair in range(pairs):
                    copy(number, pair).wait_send()


def mixer(query, forget, value, gate, floor, extra, devices):
    rows, width = query.shape[1:]
    pairs = width // PAIR
    rounds = (devices - 1).bit_length()
    early = pl.BlockSpec((1, rows, PAIR), lambda s: (0, 0, jnp.minimum(s, pairs - 1)))
    late = pl.BlockSpec((1, rows, PAIR), lambda s: (0, 0, jnp.maximum(s - rounds, 0)))
    return pl.pallas_call(
        functools.partial(mixer_kernel, devices),
        grid=(pairs + rounds,),
        in_specs=[
            early,
            early,
            early,
            late,
            pl.BlockSpec((1, PAIR), lambda s: (0, jnp.minimum(s, pairs - 1))),
            pl.BlockSpec((rows, extra.shape[1] * 3), lambda s: (0, 0)),
        ],
        out_specs=pl.BlockSpec((rows, PAIR), lambda s: (0, jnp.maximum(s - rounds, 0))),
        out_shape=jax.ShapeDtypeStruct((rows, width), jnp.bfloat16),
        scratch_shapes=[
            pltpu.VMEM((pairs, rows, PAIR), jnp.float32),
            pltpu.VMEM((pairs, rows, PAIR), jnp.bfloat16),
            pltpu.VMEM((rounds, pairs, STATE_ROWS, PAIR), jnp.bfloat16),
            pltpu.VMEM((rounds, pairs, STATE_ROWS, PAIR), jnp.bfloat16),
            pltpu.VMEM((pairs, HEAD_CHANNELS, PAIR), jnp.float32),
            pltpu.VMEM((pairs, 8, PAIR), jnp.float32),
            pltpu.VMEM((pairs, HEAD_CHANNELS, PAIR), jnp.float32),
            pltpu.VMEM((pairs, 8, PAIR), jnp.float32),
            pltpu.SemaphoreType.DMA((rounds, pairs)),
            pltpu.SemaphoreType.DMA((rounds, pairs)),
        ],
        compiler_params=pltpu.CompilerParams(collective_id=0, has_side_effects=True),
        cost_estimate=pl.CostEstimate(
            flops=rows * width * 2 * 64 * 50, bytes_accessed=rows * width * 10, transcendentals=0
        ),
    )(
        query,
        forget,
        value,
        gate,
        floor.reshape(1, width),
        jnp.concatenate(three_parts(extra), axis=1),
    )


def slots_of(hit, width):
    position = jnp.where(hit, jnp.cumsum(hit.astype(jnp.int32), axis=0) - 1, -1)
    rows, kinds = hit.shape
    return (position[:, :, None] == jnp.arange(width, dtype=jnp.int32)).reshape(
        rows, kinds * width
    )


def pick_rows(chosen, rows):
    return lax.dot_general(
        chosen.astype(jnp.bfloat16),
        rows,
        (((0,), (0,)), ((), ())),
        preferred_element_type=jnp.float32,
    ).astype(jnp.bfloat16)


def weigh_rows(weights, rows):
    high = weights.astype(jnp.bfloat16)
    low = (weights - high.astype(jnp.float32)).astype(jnp.bfloat16)
    return jnp.dot(high, rows, preferred_element_type=jnp.float32) + jnp.dot(
        low, rows, preferred_element_type=jnp.float32
    )


def per_device(
    query_weight,
    forget_preactivation,
    written_input,
    output_gate_logit,
    forget_floor,
    extra_log_decay,
    residual,
    output_weight,
    norm_scale_vector,
    expert_gate_weight,
    expert_up_weight,
    expert_down_weight,
    routes,
    routing_weight,
):
    seq_count, tok_rows, mix_width = query_weight.shape
    model_width = output_weight.shape[1]
    place = lax.axis_index("sp")
    devices = lax.axis_size("sp")
    groups = devices // GROUP
    capacity = 4 * tok_rows // devices
    group_capacity = 2 * capacity
    my_group, my_local = place // GROUP, place % GROUP

    copies = lax.axis_size("dp")
    my_copy = lax.axis_index("dp")
    shares = output_weight
    step = copies // 2
    order = [0]
    while step:
        other = lax.ppermute(shares, "dp", [(d, d ^ step) for d in range(copies)])
        shares = jnp.concatenate([shares, other], axis=0)
        order = order + [held ^ step for held in order]
        step //= 2

    picks = routes.reshape(tok_rows, 2)
    weights = routing_weight.reshape(tok_rows, 2)
    relative = (picks[:, :1] // GROUP - my_group + groups) % groups
    own_local = jnp.where(relative == 0, picks % GROUP, -1)
    peers = jnp.arange(GROUP, dtype=jnp.int32) ^ my_local

    def plan(local, share):
        first = local[:, :1] == peers
        second = local[:, 1:] == peers
        chosen = slots_of(first | second, capacity)
        weight = jnp.where(first, share[:, :1], 0.0) + jnp.where(second, share[:, 1:], 0.0)
        return chosen, jnp.where(chosen, jnp.repeat(weight, capacity, axis=1), 0.0)

    plans = [plan(own_local, weights)]
    crossing = slots_of(
        relative == jnp.arange(1, groups, dtype=jnp.int32)[None, :], group_capacity
    )
    notes = jnp.concatenate([(picks % GROUP + 1).astype(jnp.float32), weights], axis=1)
    noted = lax.dot_general(
        crossing.astype(jnp.float32), notes, (((0,), (0,)), ((), ())), precision=HIGHEST
    )

    def hop(array, distance):
        pairs = [(d, (d + GROUP * distance) % devices) for d in range(devices)]
        return lax.ppermute(array, "sp", pairs)

    def part(array, number, size):
        return lax.slice_in_dim(array, number * size, (number + 1) * size, axis=0)

    for distance in range(1, groups):
        told = hop(part(noted, distance - 1, group_capacity), distance)
        plans.append(plan(jnp.round(told[:, :2]).astype(jnp.int32) - 1, told[:, 2:]))

    extra = lax.dynamic_slice_in_dim(extra_log_decay[0], place * tok_rows, tok_rows, 0)
    mixer_out = mixer(
        query_weight,
        forget_preactivation,
        written_input,
        output_gate_logit,
        forget_floor,
        extra,
        devices,
    )
    share_width = mix_width // copies
    mixer_out = jnp.concatenate(
        [
            lax.dynamic_slice_in_dim(mixer_out, (my_copy ^ held) * share_width, share_width, 1)
            for held in order
        ],
        axis=1,
    )
    projected = jnp.dot(mixer_out, shares, preferred_element_type=jnp.float32)
    updated = (residual.reshape(tok_rows, model_width).astype(jnp.float32) + projected).astype(
        jnp.bfloat16
    )
    widened = updated.astype(jnp.float32)
    normed = (
        widened
        * lax.rsqrt(jnp.mean(widened * widened, axis=-1, keepdims=True) + 1e-06)
        * norm_scale_vector
    ).astype(jnp.bfloat16)

    leaving = pick_rows(crossing, normed)
    tokens = [normed] + [
        hop(part(leaving, distance - 1, group_capacity), distance)
        for distance in range(1, groups)
    ]

    def swap(array):
        blocks = [part(array, 0, capacity)]
        for flip in range(1, GROUP):
            pairs = [(d, d ^ flip) for d in range(devices)]
            blocks.append(lax.ppermute(part(array, flip, capacity), "sp", pairs))
        return jnp.concatenate(blocks, axis=0)

    def experts(rows):
        gated = jnp.dot(rows, expert_gate_weight[0], preferred_element_type=jnp.float32)
        upward = jnp.dot(rows, expert_up_weight[0], preferred_element_type=jnp.float32)
        hidden = (jax.nn.silu(gated) * upward).astype(jnp.bfloat16)
        return jnp.dot(
            hidden, expert_down_weight[0], preferred_element_type=jnp.float32
        ).astype(jnp.bfloat16)

    returned = [
        swap(experts(swap(pick_rows(chosen, rows)))) for (chosen, _), rows in zip(plans, tokens)
    ]
    back = [
        hop(weigh_rows(plans[d][1], returned[d]).astype(jnp.bfloat16), groups - d)
        for d in range(1, groups)
    ]
    summed = weigh_rows(plans[0][1], returned[0])
    if back:
        summed = summed + jnp.dot(
            crossing.astype(jnp.bfloat16),
            jnp.concatenate(back, axis=0),
            preferred_element_type=jnp.float32,
        )
    layer_out = (widened + summed).astype(jnp.bfloat16)
    return layer_out.reshape(seq_count, tok_rows, model_width)


def solution(mesh):
    placed = (
        P("dp", "sp", None),
        P("dp", "sp", None),
        P("dp", "sp", None),
        P("dp", "sp", None),
        P(),
        P("dp", None, None),
        P("dp", "sp", None),
        P("dp", None),
        P(),
        P("sp", None, None),
        P("sp", None, None),
        P("sp", None, None),
        P("dp", "sp", None),
        P("dp", "sp", None),
    )
    return jax.shard_map(
        per_device, mesh=mesh, in_specs=placed, out_specs=P("dp", "sp", None), check_vma=False
    )
```

```python
import functools

import jax
import jax.numpy as jnp
from jax import lax
from jax.experimental import pallas as pl
from jax.experimental.pallas import tpu as pltpu
from jax.sharding import PartitionSpec as P


HEAD_CHANNELS = 64
BLOCK = 64
PAIR = 2 * HEAD_CHANNELS
STATE_ROWS = 80
GROUP = 4
HIGHEST = lax.Precision.HIGHEST


def iota(shape, axis):
    return lax.broadcasted_iota(jnp.int32, shape, axis)


def dot_bf16(a, b, dims=((1,), (0,))):
    return lax.dot_general(
        a.astype(jnp.bfloat16),
        b.astype(jnp.bfloat16),
        (dims, ((), ())),
        preferred_element_type=jnp.float32,
    )


def three_parts(value):
    high = value.astype(jnp.bfloat16)
    rest = value - high.astype(jnp.float32)
    middle = rest.astype(jnp.bfloat16)
    low = (rest - middle.astype(jnp.float32)).astype(jnp.bfloat16)
    return high, middle, low


def mixer_kernel(
    devices,
    q_ref,
    f_ref,
    v_ref,
    gate_ref,
    floor_ref,
    extra_ref,
    out_ref,
    local_ref,
    decayed_ref,
    send_ref,
    recv_ref,
    earlier_ref,
    earlier_log_ref,
    upto_ref,
    upto_log_ref,
    send_sem,
    recv_sem,
):
    rows = q_ref.shape[1]
    pairs = local_ref.shape[0]
    rounds = send_ref.shape[0]
    heads = extra_ref.shape[1] // 3
    step = pl.program_id(0)
    place = lax.axis_index("sp")
    first = iota((1, PAIR), 1) < HEAD_CHANNELS

    def copy(number, pair):
        return pltpu.make_async_remote_copy(
            src_ref=send_ref.at[number, pair],
            dst_ref=recv_ref.at[number, pair],
            send_sem=send_sem.at[number, pair],
            recv_sem=recv_sem.at[number, pair],
            device_id={"sp": lax.rem(place + 2**number, devices)},
            device_id_type=pl.DeviceIdType.MESH,
        )

    def pack(number, pair, state, total):
        high, middle, low = three_parts(total)
        row = iota((STATE_ROWS - HEAD_CHANNELS, PAIR), 0)
        logs = jnp.where(
            row == 0,
            high.astype(jnp.float32),
            jnp.where(
                row == 1,
                middle.astype(jnp.float32),
                jnp.where(row == 2, low.astype(jnp.float32), 0.0),
            ),
        )
        send_ref[number, pair] = jnp.concatenate([state, logs], axis=0).astype(jnp.bfloat16)

    @pl.when(step == 0)
    def _():
        barrier = pltpu.get_barrier_semaphore()
        for number in range(rounds):
            for other in (place + 2**number, place + devices - 2**number):
                pl.semaphore_signal(
                    barrier,
                    inc=1,
                    device_id={"sp": lax.rem(other, devices)},
                    device_id_type=pl.DeviceIdType.MESH,
                )
        pl.semaphore_wait(barrier, 2 * rounds)

    @pl.when(step < pairs)
    def _():
        pair = step
        blocks = rows // BLOCK
        spread = (
            iota((3 * heads, PAIR), 0) % heads
            == 2 * pair + iota((3 * heads, PAIR), 1) // HEAD_CHANNELS
        ).astype(jnp.float32)
        extra = dot_bf16(extra_ref[...], spread)
        same_head = (
            iota((PAIR, PAIR), 0) // HEAD_CHANNELS == iota((PAIR, PAIR), 1) // HEAD_CHANNELS
        )
        lower = (iota((BLOCK, 3 * BLOCK), 0) >= iota((BLOCK, 3 * BLOCK), 1) % BLOCK).astype(
            jnp.float32
        )
        causal = iota((2 * BLOCK, BLOCK), 0) % BLOCK >= iota((2 * BLOCK, BLOCK), 1)
        open_share = 1.0 - floor_ref[...]
        keys = []
        logs = []
        for block in range(blocks):
            at = slice(block * BLOCK, (block + 1) * BLOCK)
            k = open_share / (1.0 + jnp.exp(f_ref[0, at, :].astype(jnp.float32)))
            keys.append(k)
            logs.append(
                jnp.concatenate(three_parts(jnp.log1p(-k) + extra[at]), axis=0)
            )
        sums = dot_bf16(lower, jnp.concatenate(logs, axis=1))
        state = jnp.zeros((PAIR, PAIR), jnp.float32)
        before = jnp.zeros((1, PAIR), jnp.float32)
        for block in range(blocks):
            at = slice(block * BLOCK, (block + 1) * BLOCK)
            q = q_ref[0, at, :].astype(jnp.float32)
            v = v_ref[0, at, :]
            k = keys[block]
            q = q / (1.0 + jnp.exp(-q))
            cumulative = sums[:, block * PAIR : (block + 1) * PAIR]
            closing = cumulative[BLOCK - 1 :, :]
            q_decayed = q * jnp.exp(cumulative)
            k_grown = k * jnp.exp(-cumulative)
            k_closing = k * jnp.exp(closing - cumulative)
            stacked = jnp.concatenate(
                [jnp.where(first, q_decayed, 0.0), jnp.where(first, 0.0, q_decayed)], axis=0
            )
            scores = jnp.where(causal, dot_bf16(stacked, k_grown, ((1,), (1,))), 0.0)
            inner = dot_bf16(scores, v)
            inner = jnp.where(first, inner[:BLOCK], inner[BLOCK:])
            local_ref[pair, at, :] = inner + dot_bf16(q_decayed, state, ((1,), (1,)))
            decayed_ref[pair, at, :] = (q_decayed * jnp.exp(before)).astype(jnp.bfloat16)
            state = state * jnp.exp(closing) + jnp.where(
                same_head, dot_bf16(v, k_closing, ((0,), (0,))), 0.0
            )
            before = before + closing
        folded = jnp.where(first, state[:HEAD_CHANNELS], state[HEAD_CHANNELS:])
        upto_ref[pair] = folded
        upto_log_ref[pair] = jnp.broadcast_to(before, (8, PAIR))
        earlier_ref[pair] = jnp.zeros((HEAD_CHANNELS, PAIR), jnp.float32)
        earlier_log_ref[pair] = jnp.zeros((8, PAIR), jnp.float32)

        @pl.when(place + 1 < devices)
        def _():
            pack(0, pair, folded, before)
            copy(0, pair).start()

    def merge(number):
        distance = 2**number
        pair = step - 1 - number

        @pl.when((pair >= 0) & (pair < pairs))
        def _():
            @pl.when(place >= distance)
            def _():
                copy(number, pair).wait_recv()
                item = recv_ref[number, pair].astype(jnp.float32)
                state = item[:HEAD_CHANNELS]
                total = jnp.sum(item[HEAD_CHANNELS:], axis=0, keepdims=True)
                log = earlier_log_ref[pair][:1]
                earlier_ref[pair] = state * jnp.exp(log) + earlier_ref[pair]
                earlier_log_ref[pair] = jnp.broadcast_to(log + total, (8, PAIR))
                if number + 1 < rounds:
                    log = upto_log_ref[pair][:1]
                    upto_ref[pair] = state * jnp.exp(log) + upto_ref[pair]
                    upto_log_ref[pair] = jnp.broadcast_to(log + total, (8, PAIR))

            if number + 1 < rounds:

                @pl.when(place + 2 * distance < devices)
                def _():
                    pack(number + 1, pair, upto_ref[pair], upto_log_ref[pair][:1])
                    copy(number + 1, pair).start()

    for number in range(rounds):
        merge(number)

    pair = step - rounds

    @pl.when(pair >= 0)
    def _():
        state = earlier_ref[pair]
        state = jnp.concatenate(
            [jnp.where(first, state, 0.0), jnp.where(first, 0.0, state)], axis=0
        )
        value = local_ref[pair] + dot_bf16(decayed_ref[pair], state, ((1,), (1,)))
        same_head = (
            iota((2 * PAIR, PAIR), 0) // HEAD_CHANNELS % 2 == iota((2 * PAIR, PAIR), 1) // HEAD_CHANNELS
        ).astype(jnp.float32)
        square = value * value
        high = square.astype(jnp.bfloat16)
        low = (square - high.astype(jnp.float32)).astype(jnp.bfloat16)
        mean = dot_bf16(jnp.concatenate([high, low], axis=1), same_head) * (1.0 / HEAD_CHANNELS)
        gate = gate_ref[0].astype(jnp.float32)
        gate = gate / (1.0 + jnp.exp(-gate))
        out_ref[...] = (value * lax.rsqrt(mean + 1e-06) * gate).astype(jnp.bfloat16)

    @pl.when(step == pairs + rounds - 1)
    def _():
        for number in range(rounds):

            @pl.when(place + 2**number < devices)
            def _():
                for pair in range(pairs):
                    copy(number, pair).wait_send()


def mixer(query, forget, value, gate, floor, extra, devices):
    rows, width = query.shape[1:]
    pairs = width // PAIR
    rounds = (devices - 1).bit_length()
    early = pl.BlockSpec((1, rows, PAIR), lambda s: (0, 0, jnp.minimum(s, pairs - 1)))
    late = pl.BlockSpec((1, rows, PAIR), lambda s: (0, 0, jnp.maximum(s - rounds, 0)))
    return pl.pallas_call(
        functools.partial(mixer_kernel, devices),
        grid=(pairs + rounds,),
        in_specs=[
            early,
            early,
            early,
            late,
            pl.BlockSpec((1, PAIR), lambda s: (0, jnp.minimum(s, pairs - 1))),
            pl.BlockSpec((rows, extra.shape[1] * 3), lambda s: (0, 0)),
        ],
        out_specs=pl.BlockSpec((rows, PAIR), lambda s: (0, jnp.maximum(s - rounds, 0))),
        out_shape=jax.ShapeDtypeStruct((rows, width), jnp.bfloat16),
        scratch_shapes=[
            pltpu.VMEM((pairs, rows, PAIR), jnp.float32),
            pltpu.VMEM((pairs, rows, PAIR), jnp.bfloat16),
            pltpu.VMEM((rounds, pairs, STATE_ROWS, PAIR), jnp.bfloat16),
            pltpu.VMEM((rounds, pairs, STATE_ROWS, PAIR), jnp.bfloat16),
            pltpu.VMEM((pairs, HEAD_CHANNELS, PAIR), jnp.float32),
            pltpu.VMEM((pairs, 8, PAIR), jnp.float32),
            pltpu.VMEM((pairs, HEAD_CHANNELS, PAIR), jnp.float32),
            pltpu.VMEM((pairs, 8, PAIR), jnp.float32),
            pltpu.SemaphoreType.DMA((rounds, pairs)),
            pltpu.SemaphoreType.DMA((rounds, pairs)),
        ],
        compiler_params=pltpu.CompilerParams(collective_id=0, has_side_effects=True),
        cost_estimate=pl.CostEstimate(
            flops=rows * width * 2 * 64 * 50, bytes_accessed=rows * width * 10, transcendentals=0
        ),
    )(
        query,
        forget,
        value,
        gate,
        floor.reshape(1, width),
        jnp.concatenate(three_parts(extra), axis=1),
    )


def positions_of(hit):
    rows = hit.shape[0]
    lower = (iota((rows, rows), 0) >= iota((rows, rows), 1)).astype(jnp.bfloat16)
    count = jnp.dot(lower, hit.astype(jnp.bfloat16), preferred_element_type=jnp.float32)
    return jnp.where(hit, count - 1.0, -1.0)


def spread_kinds(values, width):
    kinds = values.shape[1]
    wide = (iota((kinds, kinds * width), 1) // width == iota((kinds, kinds * width), 0)).astype(
        jnp.bfloat16
    )
    return jnp.dot(values.astype(jnp.bfloat16), wide, preferred_element_type=jnp.float32)


def pick_rows(chosen, rows):
    return lax.dot_general(
        chosen.astype(jnp.bfloat16),
        rows,
        (((0,), (0,)), ((), ())),
        preferred_element_type=jnp.float32,
    ).astype(jnp.bfloat16)


def weigh_rows(weights, rows):
    high, low = weights
    return jnp.dot(high, rows, preferred_element_type=jnp.float32) + jnp.dot(
        low, rows, preferred_element_type=jnp.float32
    )


def per_device(
    query_weight,
    forget_preactivation,
    written_input,
    output_gate_logit,
    forget_floor,
    extra_log_decay,
    residual,
    output_weight,
    norm_scale_vector,
    expert_gate_weight,
    expert_up_weight,
    expert_down_weight,
    routes,
    routing_weight,
):
    seq_count, tok_rows, mix_width = query_weight.shape
    model_width = output_weight.shape[1]
    place = lax.axis_index("sp")
    devices = lax.axis_size("sp")
    groups = devices // GROUP
    capacity = 4 * tok_rows // devices
    group_capacity = 2 * capacity
    my_group, my_local = place // GROUP, place % GROUP

    copies = lax.axis_size("dp")
    my_copy = lax.axis_index("dp")

    picks = routes.reshape(tok_rows, 2)
    weights = routing_weight.reshape(tok_rows, 2)
    relative = (picks[:, :1] // GROUP - my_group + groups) % groups
    own_local = jnp.where(relative == 0, picks % GROUP, -1)
    peers = jnp.arange(GROUP, dtype=jnp.int32) ^ my_local

    def plan(local):
        first = local[:, :1] == peers
        second = local[:, 1:] == peers
        position = positions_of(first | second)
        rows, kinds = position.shape
        slot = (iota((rows, kinds * capacity), 1) % capacity).astype(jnp.float32)
        chosen = spread_kinds(position, capacity) == slot
        return lax.optimization_barrier(chosen.astype(jnp.bfloat16))

    def weigh_tables(local, share, chosen):
        weight = jnp.where(local[:, :1] == peers, share[:, :1], 0.0) + jnp.where(
            local[:, 1:] == peers, share[:, 1:], 0.0
        )
        high = weight.astype(jnp.bfloat16)
        low = (weight - high.astype(jnp.float32)).astype(jnp.bfloat16)
        return lax.optimization_barrier(
            tuple(
                (spread_kinds(half, capacity) * chosen.astype(jnp.float32)).astype(jnp.bfloat16)
                for half in (high, low)
            )
        )

    own_plan = plan(own_local)
    leaves = positions_of(relative == jnp.arange(1, groups, dtype=jnp.int32)[None, :])
    place_in_group = iota((tok_rows, group_capacity), 1).astype(jnp.float32)
    crossing = jnp.concatenate(
        [leaves[:, number : number + 1] == place_in_group for number in range(groups - 1)], axis=1
    )
    notes = jnp.concatenate([(picks % GROUP + 1).astype(jnp.float32), weights], axis=1)
    noted = lax.dot_general(
        crossing.astype(jnp.float32), notes, (((0,), (0,)), ((), ())), precision=HIGHEST
    )

    def hop(array, distance):
        pairs = [(d, (d + GROUP * distance) % devices) for d in range(devices)]
        return lax.ppermute(array, "sp", pairs)

    def part(array, number, size):
        return lax.slice_in_dim(array, number * size, (number + 1) * size, axis=0)

    told = [
        hop(part(noted, distance - 1, group_capacity), distance)
        for distance in range(1, groups)
    ]

    extra = lax.dynamic_slice_in_dim(extra_log_decay[0], place * tok_rows, tok_rows, 0)
    mixer_out = mixer(
        query_weight,
        forget_preactivation,
        written_input,
        output_gate_logit,
        forget_floor,
        extra,
        devices,
    )

    shares = output_weight
    step = copies // 2
    order = [0]
    while step:
        other = lax.ppermute(shares, "dp", [(d, d ^ step) for d in range(copies)])
        if step == copies // 2:
            other, mixer_out = lax.optimization_barrier((other, mixer_out))
        shares = jnp.concatenate([shares, other], axis=0)
        order = order + [held ^ step for held in order]
        step //= 2

    share_width = mix_width // copies
    mixer_out = jnp.concatenate(
        [
            lax.dynamic_slice_in_dim(mixer_out, (my_copy ^ held) * share_width, share_width, 1)
            for held in order
        ],
        axis=1,
    )
    projected = jnp.dot(mixer_out, shares, preferred_element_type=jnp.float32)
    updated = (residual.reshape(tok_rows, model_width).astype(jnp.float32) + projected).astype(
        jnp.bfloat16
    )
    widened = updated.astype(jnp.float32)
    normed = (
        widened
        * lax.rsqrt(jnp.mean(widened * widened, axis=-1, keepdims=True) + 1e-06)
        * norm_scale_vector
    ).astype(jnp.bfloat16)

    def experts(rows):
        gate = jnp.dot(rows, expert_gate_weight[0], preferred_element_type=jnp.float32)
        up = jnp.dot(rows, expert_up_weight[0], preferred_element_type=jnp.float32)
        hidden = (jax.nn.silu(gate) * up).astype(jnp.bfloat16)
        return jnp.dot(
            hidden, expert_down_weight[0], preferred_element_type=jnp.float32
        ).astype(jnp.bfloat16)

    def swapped(blocks):
        moved = {
            bits: lax.ppermute(blocks[bits], "sp", [(d, d ^ bits) for d in range(devices)])
            for bits in range(GROUP - 1, 0, -1)
        }
        return [blocks[0]] + [moved[bits] for bits in range(1, GROUP)]

    def blocks_of(array):
        return [part(array, bits, capacity) for bits in range(GROUP)]

    leaving = pick_rows(crossing, normed)
    arrived = [
        hop(part(leaving, distance - 1, group_capacity), distance)
        for distance in range(1, groups)
    ]
    own_rows = pick_rows(own_plan, normed)
    late = (weights, own_plan, *told, own_rows)
    weights, own_plan, *told, own_rows = lax.optimization_barrier(late)
    own = swapped(blocks_of(own_rows))
    locals_told = [jnp.round(t[:, :2]).astype(jnp.int32) - 1 for t in told]
    plans = [plan(local) for local in locals_told]
    tables = [weigh_tables(own_local, weights, own_plan)] + [
        weigh_tables(local, t[:, 2:], chosen)
        for local, t, chosen in zip(locals_told, told, plans)
    ]
    given = [swapped(blocks_of(pick_rows(p, rows))) for p, rows in zip(plans, arrived)]
    own_made = experts(jnp.concatenate(own, axis=0))
    back = []
    for number, blocks in enumerate(given, 1):
        made = experts(jnp.concatenate(blocks, axis=0))
        made = swapped(blocks_of(made))
        total = weigh_rows(tables[number], jnp.concatenate(made, axis=0)).astype(jnp.bfloat16)
        back.append(hop(total, groups - number))
    own_made = jnp.concatenate(swapped(blocks_of(own_made)), axis=0)
    summed = weigh_rows(tables[0], own_made)
    if back:
        summed = summed + jnp.dot(
            crossing.astype(jnp.bfloat16),
            jnp.concatenate(back, axis=0),
            preferred_element_type=jnp.float32,
        )
    layer_out = (widened + summed).astype(jnp.bfloat16)
    return layer_out.reshape(seq_count, tok_rows, model_width)


def solution(mesh):
    placed = (
        P("dp", "sp", None),
        P("dp", "sp", None),
        P("dp", "sp", None),
        P("dp", "sp", None),
        P(),
        P("dp", None, None),
        P("dp", "sp", None),
        P("dp", None),
        P(),
        P("sp", None, None),
        P("sp", None, None),
        P("sp", None, None),
        P("dp", "sp", None),
        P("dp", "sp", None),
    )

    return jax.shard_map(
        per_device, mesh=mesh, in_specs=placed, out_specs=P("dp", "sp", None), check_vma=False
    )
```

```python
import functools

import jax
import jax.numpy as jnp
from jax import lax
from jax.experimental import pallas as pl
from jax.experimental.pallas import tpu as pltpu
from jax.sharding import PartitionSpec as P


HEAD_CHANNELS = 64
BLOCK = 64
PAIR = 2 * HEAD_CHANNELS
STATE_ROWS = 80
GROUP = 4
HIGHEST = lax.Precision.HIGHEST


def iota(shape, axis):
    return lax.broadcasted_iota(jnp.int32, shape, axis)


def dot_bf16(a, b, dims=((1,), (0,))):
    return lax.dot_general(
        a.astype(jnp.bfloat16),
        b.astype(jnp.bfloat16),
        (dims, ((), ())),
        preferred_element_type=jnp.float32,
    )


def three_parts(value):
    high = value.astype(jnp.bfloat16)
    rest = value - high.astype(jnp.float32)
    middle = rest.astype(jnp.bfloat16)
    low = (rest - middle.astype(jnp.float32)).astype(jnp.bfloat16)
    return high, middle, low


def mixer_kernel(
    devices,
    q_ref,
    f_ref,
    v_ref,
    gate_ref,
    floor_ref,
    extra_ref,
    share_ref,
    out_ref,
    shares_ref,
    local_ref,
    decayed_ref,
    send_ref,
    recv_ref,
    earlier_ref,
    earlier_log_ref,
    upto_ref,
    upto_log_ref,
    send_sem,
    recv_sem,
    share_send_sem,
    share_recv_sem,
    share_sem,
):
    rows = q_ref.shape[1]
    pairs = local_ref.shape[0]
    rounds = send_ref.shape[0]
    heads = extra_ref.shape[1]
    step = pl.program_id(0)
    place = lax.axis_index("sp")
    first = iota((1, PAIR), 1) < HEAD_CHANNELS
    copies = shares_ref.shape[0]
    my_copy = lax.axis_index("dp")

    def partner(source, step):
        return source + step - 2 * step * ((source // step) % 2)

    hand_overs = []
    held = [my_copy]
    stride = copies // 2
    while stride:
        hand_overs.append([(source, stride) for source in held])
        held = held + [partner(source, stride) for source in held]
        stride //= 2

    def hand_over(stage, number):
        source, stride = hand_overs[stage][number]
        return pltpu.make_async_remote_copy(
            src_ref=share_ref if number == 0 else shares_ref.at[source],
            dst_ref=shares_ref.at[source],
            send_sem=share_send_sem.at[stage, number],
            recv_sem=share_recv_sem.at[stage, number],
            device_id={"dp": partner(my_copy, stride)},
            device_id_type=pl.DeviceIdType.MESH,
        )

    def keep_share():
        return pltpu.make_async_copy(share_ref, shares_ref.at[my_copy], share_sem)

    def copy(number, pair):
        return pltpu.make_async_remote_copy(
            src_ref=send_ref.at[number, pair],
            dst_ref=recv_ref.at[number, pair],
            send_sem=send_sem.at[number, pair],
            recv_sem=recv_sem.at[number, pair],
            device_id={"sp": lax.rem(place + 2**number, devices)},
            device_id_type=pl.DeviceIdType.MESH,
        )

    def pack(number, pair, state, total):
        high, middle, low = three_parts(total)
        row = iota((STATE_ROWS - HEAD_CHANNELS, PAIR), 0)
        logs = jnp.where(
            row == 0,
            high.astype(jnp.float32),
            jnp.where(
                row == 1,
                middle.astype(jnp.float32),
                jnp.where(row == 2, low.astype(jnp.float32), 0.0),
            ),
        )
        send_ref[number, pair] = jnp.concatenate([state, logs], axis=0).astype(jnp.bfloat16)

    @pl.when(step == 0)
    def _():
        barrier = pltpu.get_barrier_semaphore()
        for number in range(rounds):
            for other in (place + 2**number, place + devices - 2**number):
                pl.semaphore_signal(
                    barrier,
                    inc=1,
                    device_id={"sp": lax.rem(other, devices)},
                    device_id_type=pl.DeviceIdType.MESH,
                )
        for group in hand_overs:
            pl.semaphore_signal(
                barrier,
                inc=1,
                device_id={"dp": partner(my_copy, group[0][1])},
                device_id_type=pl.DeviceIdType.MESH,
            )
        pl.semaphore_wait(barrier, 2 * rounds + len(hand_overs))
        keep_share().start()
        for stage in range(len(hand_overs)):
            hand_over(stage, 0).start()

    @pl.when(step < pairs)
    def _():
        pair = step
        blocks = rows // BLOCK
        spread = (
            iota((heads, PAIR), 0) == 2 * pair + iota((heads, PAIR), 1) // HEAD_CHANNELS
        ).astype(jnp.float32)
        high, middle, low = (dot_bf16(third, spread) for third in three_parts(extra_ref[...]))
        extra = high + (middle + low)
        same_head = (
            iota((PAIR, PAIR), 0) // HEAD_CHANNELS == iota((PAIR, PAIR), 1) // HEAD_CHANNELS
        )
        lower = (iota((BLOCK, 3 * BLOCK), 0) >= iota((BLOCK, 3 * BLOCK), 1) % BLOCK).astype(
            jnp.float32
        )
        causal = iota((2 * BLOCK, BLOCK), 0) % BLOCK >= iota((2 * BLOCK, BLOCK), 1)
        open_share = 1.0 - floor_ref[...]
        keys = []
        logs = []
        for block in range(blocks):
            at = slice(block * BLOCK, (block + 1) * BLOCK)
            k = open_share / (1.0 + jnp.exp(f_ref[0, at, :].astype(jnp.float32)))
            keys.append(k)
            logs.append(
                jnp.concatenate(three_parts(jnp.log1p(-k) + extra[at]), axis=0)
            )
        sums = dot_bf16(lower, jnp.concatenate(logs, axis=1))
        state = jnp.zeros((PAIR, PAIR), jnp.float32)
        before = jnp.zeros((1, PAIR), jnp.float32)
        for block in range(blocks):
            at = slice(block * BLOCK, (block + 1) * BLOCK)
            q = q_ref[0, at, :].astype(jnp.float32)
            v = v_ref[0, at, :]
            k = keys[block]
            q = q / (1.0 + jnp.exp(-q))
            cumulative = sums[:, block * PAIR : (block + 1) * PAIR]
            closing = cumulative[BLOCK - 1 :, :]
            q_decayed = q * jnp.exp(cumulative)
            k_grown = k * jnp.exp(-cumulative)
            k_closing = k * jnp.exp(closing - cumulative)
            stacked = jnp.concatenate(
                [jnp.where(first, q_decayed, 0.0), jnp.where(first, 0.0, q_decayed)], axis=0
            )
            scores = jnp.where(causal, dot_bf16(stacked, k_grown, ((1,), (1,))), 0.0)
            inner = dot_bf16(scores, v)
            inner = jnp.where(first, inner[:BLOCK], inner[BLOCK:])
            local_ref[pair, at, :] = inner + dot_bf16(q_decayed, state, ((1,), (1,)))
            decayed_ref[pair, at, :] = (q_decayed * jnp.exp(before)).astype(jnp.bfloat16)
            state = state * jnp.exp(closing) + jnp.where(
                same_head, dot_bf16(v, k_closing, ((0,), (0,))), 0.0
            )
            before = before + closing
        folded = jnp.where(first, state[:HEAD_CHANNELS], state[HEAD_CHANNELS:])
        upto_ref[pair] = folded
        upto_log_ref[pair] = jnp.broadcast_to(before, (8, PAIR))
        earlier_ref[pair] = jnp.zeros((HEAD_CHANNELS, PAIR), jnp.float32)
        earlier_log_ref[pair] = jnp.zeros((8, PAIR), jnp.float32)

        @pl.when(place + 1 < devices)
        def _():
            pack(0, pair, folded, before)
            copy(0, pair).start()

    def merge(number):
        distance = 2**number
        pair = step - 1 - number

        @pl.when((pair >= 0) & (pair < pairs))
        def _():
            @pl.when(place >= distance)
            def _():
                copy(number, pair).wait_recv()
                item = recv_ref[number, pair].astype(jnp.float32)
                state = item[:HEAD_CHANNELS]
                total = jnp.sum(item[HEAD_CHANNELS:], axis=0, keepdims=True)
                log = earlier_log_ref[pair][:1]
                earlier_ref[pair] = state * jnp.exp(log) + earlier_ref[pair]
                earlier_log_ref[pair] = jnp.broadcast_to(log + total, (8, PAIR))
                if number + 1 < rounds:
                    log = upto_log_ref[pair][:1]
                    upto_ref[pair] = state * jnp.exp(log) + upto_ref[pair]
                    upto_log_ref[pair] = jnp.broadcast_to(log + total, (8, PAIR))

            if number + 1 < rounds:

                @pl.when(place + 2 * distance < devices)
                def _():
                    pack(number + 1, pair, upto_ref[pair], upto_log_ref[pair][:1])
                    copy(number + 1, pair).start()

    for number in range(rounds):
        merge(number)

    pair = step - rounds

    @pl.when(pair >= 0)
    def _():
        state = earlier_ref[pair]
        state = jnp.concatenate(
            [jnp.where(first, state, 0.0), jnp.where(first, 0.0, state)], axis=0
        )
        value = local_ref[pair] + dot_bf16(decayed_ref[pair], state, ((1,), (1,)))
        same_head = (
            iota((2 * PAIR, PAIR), 0) // HEAD_CHANNELS % 2 == iota((2 * PAIR, PAIR), 1) // HEAD_CHANNELS
        ).astype(jnp.float32)
        square = value * value
        high = square.astype(jnp.bfloat16)
        low = (square - high.astype(jnp.float32)).astype(jnp.bfloat16)
        mean = dot_bf16(jnp.concatenate([high, low], axis=1), same_head) * (1.0 / HEAD_CHANNELS)
        gate = gate_ref[0].astype(jnp.float32)
        gate = gate / (1.0 + jnp.exp(-gate))
        out_ref[...] = (value * lax.rsqrt(mean + 1e-06) * gate).astype(jnp.bfloat16)

    @pl.when(step == pairs + rounds - 2)
    def _():
        for stage in range(1, len(hand_overs)):
            for number in range(len(hand_overs[stage - 1])):
                hand_over(stage - 1, number).wait_recv()
            for number in range(1, len(hand_overs[stage])):
                hand_over(stage, number).start()

    @pl.when(step == pairs + rounds - 1)
    def _():
        keep_share().wait()
        for stage, group in enumerate(hand_overs):
            for number in range(len(group)):
                hand_over(stage, number).wait_send()
                if stage == len(hand_overs) - 1:
                    hand_over(stage, number).wait_recv()
        for number in range(rounds):

            @pl.when(place + 2**number < devices)
            def _():
                for pair in range(pairs):
                    copy(number, pair).wait_send()


def mixer(query, forget, value, gate, floor, extra, share, devices, copies):
    rows, width = query.shape[1:]
    pairs = width // PAIR
    rounds = (devices - 1).bit_length()
    early = pl.BlockSpec((1, rows, PAIR), lambda s: (0, 0, jnp.minimum(s, pairs - 1)))
    late = pl.BlockSpec((1, rows, PAIR), lambda s: (0, 0, jnp.maximum(s - rounds, 0)))
    return pl.pallas_call(
        functools.partial(mixer_kernel, devices),
        grid=(pairs + rounds,),
        in_specs=[
            early,
            early,
            early,
            late,
            pl.BlockSpec((1, PAIR), lambda s: (0, jnp.minimum(s, pairs - 1))),
            pl.BlockSpec((rows, extra.shape[1]), lambda s: (0, 0)),
            pl.BlockSpec(memory_space=pltpu.VMEM),
        ],
        out_specs=[
            pl.BlockSpec((rows, PAIR), lambda s: (0, jnp.maximum(s - rounds, 0))),
            pl.BlockSpec(memory_space=pl.ANY),
        ],
        out_shape=[
            jax.ShapeDtypeStruct((rows, width), jnp.bfloat16),
            jax.ShapeDtypeStruct((copies,) + share.shape, share.dtype),
        ],
        scratch_shapes=[
            pltpu.VMEM((pairs, rows, PAIR), jnp.float32),
            pltpu.VMEM((pairs, rows, PAIR), jnp.bfloat16),
            pltpu.VMEM((rounds, pairs, STATE_ROWS, PAIR), jnp.bfloat16),
            pltpu.VMEM((rounds, pairs, STATE_ROWS, PAIR), jnp.bfloat16),
            pltpu.VMEM((pairs, HEAD_CHANNELS, PAIR), jnp.float32),
            pltpu.VMEM((pairs, 8, PAIR), jnp.float32),
            pltpu.VMEM((pairs, HEAD_CHANNELS, PAIR), jnp.float32),
            pltpu.VMEM((pairs, 8, PAIR), jnp.float32),
            pltpu.SemaphoreType.DMA((rounds, pairs)),
            pltpu.SemaphoreType.DMA((rounds, pairs)),
            pltpu.SemaphoreType.DMA((copies.bit_length() - 1, copies // 2)),
            pltpu.SemaphoreType.DMA((copies.bit_length() - 1, copies // 2)),
            pltpu.SemaphoreType.DMA,
        ],
        compiler_params=pltpu.CompilerParams(collective_id=0, has_side_effects=True),
        cost_estimate=pl.CostEstimate(
            flops=rows * width * 2 * 64 * 50, bytes_accessed=rows * width * 10, transcendentals=0
        ),
    )(
        query,
        forget,
        value,
        gate,
        floor.reshape(1, width),
        extra,
        share,
    )


def positions_of(hit):
    rows = hit.shape[0]
    lower = (iota((rows, rows), 0) >= iota((rows, rows), 1)).astype(jnp.bfloat16)
    count = jnp.dot(lower, hit.astype(jnp.bfloat16), preferred_element_type=jnp.float32)
    return jnp.where(hit, count - 1.0, -1.0)


def spread_kinds(values, width):
    kinds = values.shape[1]
    wide = (iota((kinds, kinds * width), 1) // width == iota((kinds, kinds * width), 0)).astype(
        jnp.bfloat16
    )
    return jnp.dot(values.astype(jnp.bfloat16), wide, preferred_element_type=jnp.float32)


def pick_rows(chosen, rows):
    return lax.dot_general(
        chosen.astype(jnp.bfloat16),
        rows,
        (((0,), (0,)), ((), ())),
        preferred_element_type=jnp.float32,
    ).astype(jnp.bfloat16)


def weigh_rows(weights, rows):
    high, low = weights
    return jnp.dot(high, rows, preferred_element_type=jnp.float32) + jnp.dot(
        low, rows, preferred_element_type=jnp.float32
    )


def per_device(
    query_weight,
    forget_preactivation,
    written_input,
    output_gate_logit,
    forget_floor,
    extra_log_decay,
    residual,
    output_weight,
    norm_scale_vector,
    expert_gate_weight,
    expert_up_weight,
    expert_down_weight,
    routes,
    routing_weight,
):
    seq_count, tok_rows, mix_width = query_weight.shape
    model_width = output_weight.shape[1]
    place = lax.axis_index("sp")
    devices = lax.axis_size("sp")
    groups = devices // GROUP
    capacity = 4 * tok_rows // devices
    group_capacity = 2 * capacity
    my_group, my_local = place // GROUP, place % GROUP

    copies = lax.axis_size("dp")
    picks = routes.reshape(tok_rows, 2)
    weights = routing_weight.reshape(tok_rows, 2)
    relative = (picks[:, :1] // GROUP - my_group + groups) % groups
    own_local = jnp.where(relative == 0, picks % GROUP, -1)
    peers = jnp.arange(GROUP, dtype=jnp.int32) ^ my_local

    def plan(local):
        first = local[:, :1] == peers
        second = local[:, 1:] == peers
        position = positions_of(first | second)
        rows, kinds = position.shape
        slot = (iota((rows, kinds * capacity), 1) % capacity).astype(jnp.float32)
        chosen = spread_kinds(position, capacity) == slot
        return lax.optimization_barrier(chosen.astype(jnp.bfloat16))

    def weigh_tables(local, share, chosen):
        weight = jnp.where(local[:, :1] == peers, share[:, :1], 0.0) + jnp.where(
            local[:, 1:] == peers, share[:, 1:], 0.0
        )
        high = weight.astype(jnp.bfloat16)
        low = (weight - high.astype(jnp.float32)).astype(jnp.bfloat16)
        return lax.optimization_barrier(
            tuple(
                (spread_kinds(half, capacity) * chosen.astype(jnp.float32)).astype(jnp.bfloat16)
                for half in (high, low)
            )
        )

    leaves = positions_of(relative == jnp.arange(1, groups, dtype=jnp.int32)[None, :])
    place_in_group = iota((tok_rows, group_capacity), 1).astype(jnp.float32)
    crossing = jnp.concatenate(
        [leaves[:, number : number + 1] == place_in_group for number in range(groups - 1)], axis=1
    )
    notes = jnp.concatenate([(picks % GROUP + 1).astype(jnp.float32), weights], axis=1)
    noted = lax.dot_general(
        crossing.astype(jnp.float32), notes, (((0,), (0,)), ((), ())), precision=HIGHEST
    )

    def hop(array, distance):
        pairs = [(d, (d + GROUP * distance) % devices) for d in range(devices)]
        return lax.ppermute(array, "sp", pairs)

    def part(array, number, size):
        return lax.slice_in_dim(array, number * size, (number + 1) * size, axis=0)

    extra = lax.dynamic_slice_in_dim(extra_log_decay[0], place * tok_rows, tok_rows, 0)
    mixer_out, shares = mixer(
        query_weight,
        forget_preactivation,
        written_input,
        output_gate_logit,
        forget_floor,
        extra,
        output_weight,
        devices,
        copies,
    )

    shares = shares.reshape(mix_width, model_width)
    projected = jnp.dot(mixer_out, shares, preferred_element_type=jnp.float32)
    updated = (residual.reshape(tok_rows, model_width).astype(jnp.float32) + projected).astype(
        jnp.bfloat16
    )
    widened = updated.astype(jnp.float32)
    normed = (
        widened
        * lax.rsqrt(jnp.mean(widened * widened, axis=-1, keepdims=True) + 1e-06)
        * norm_scale_vector
    ).astype(jnp.bfloat16)

    def experts(rows):
        gate = jnp.dot(rows, expert_gate_weight[0], preferred_element_type=jnp.float32)
        up = jnp.dot(rows, expert_up_weight[0], preferred_element_type=jnp.float32)
        hidden = lax.optimization_barrier((jax.nn.silu(gate) * up).astype(jnp.bfloat16))
        return jnp.dot(
            hidden, expert_down_weight[0], preferred_element_type=jnp.float32
        ).astype(jnp.bfloat16)

    def swapped(blocks):
        moved = {
            bits: lax.ppermute(blocks[bits], "sp", [(d, d ^ bits) for d in range(devices)])
            for bits in range(GROUP - 1, 0, -1)
        }
        return [blocks[0]] + [moved[bits] for bits in range(1, GROUP)]

    def blocks_of(array):
        return [part(array, bits, capacity) for bits in range(GROUP)]

    leaving = pick_rows(crossing, normed)
    arrived = [
        hop(part(leaving, distance - 1, group_capacity), distance)
        for distance in range(1, groups)
    ]
    own_local, late_normed = lax.optimization_barrier((own_local, normed))
    own_plan = plan(own_local)
    own_rows = pick_rows(own_plan, late_normed)
    late = (weights, own_plan, noted, own_rows)
    weights, own_plan, noted, own_rows = lax.optimization_barrier(late)
    told = [
        hop(part(noted, distance - 1, group_capacity), distance)
        for distance in range(1, groups)
    ]

    own = swapped(blocks_of(own_rows))
    locals_told = [jnp.round(t[:, :2]).astype(jnp.int32) - 1 for t in told]
    plans = [plan(local) for local in locals_told]
    tables = [weigh_tables(own_local, weights, own_plan)] + [
        weigh_tables(local, t[:, 2:], chosen)
        for local, t, chosen in zip(locals_told, told, plans)
    ]
    given = [swapped(blocks_of(pick_rows(p, rows))) for p, rows in zip(plans, arrived)]
    own_made = experts(jnp.concatenate(own, axis=0))
    back = []
    for number, blocks in enumerate(given, 1):
        middle = GROUP // 2
        near = experts(jnp.concatenate(blocks[:middle], axis=0))
        across_z = experts(jnp.concatenate(blocks[middle:], axis=0))
        made = swapped(
            [part(near, bits, capacity) for bits in range(middle)]
            + [part(across_z, bits, capacity) for bits in range(GROUP - middle)]
        )
        total = weigh_rows(tables[number], jnp.concatenate(made, axis=0)).astype(jnp.bfloat16)
        back.append(hop(total, groups - number))
    own_made = jnp.concatenate(swapped(blocks_of(own_made)), axis=0)
    summed = weigh_rows(tables[0], own_made)
    if back:
        summed = summed + jnp.dot(
            crossing.astype(jnp.bfloat16),
            jnp.concatenate(back, axis=0),
            preferred_element_type=jnp.float32,
        )
    layer_out = (widened + summed).astype(jnp.bfloat16)
    return layer_out.reshape(seq_count, tok_rows, model_width)


def solution(mesh):
    placed = (
        P("dp", "sp", None),
        P("dp", "sp", None),
        P("dp", "sp", None),
        P("dp", "sp", None),
        P(),
        P("dp", None, None),
        P("dp", "sp", None),
        P("dp", None),
        P(),
        P("sp", None, None),
        P("sp", None, None),
        P("sp", None, None),
        P("dp", "sp", None),
        P("dp", "sp", None),
    )

    return jax.shard_map(
        per_device, mesh=mesh, in_specs=placed, out_specs=P("dp", "sp", None), check_vma=False
    )
```
